32 devices in a mesh: grp: 2 (over y), sp: 4 (over z), tp: 4 (over x, core).
Axes of the slice: x: 2, y: 2, z: 4, core: 2. Of those that a mesh axis runs over, the one named last changes fastest.
Arguments:
- tokens: bfloat16 [4096, 2048], P(('grp', 'sp'), 'tp'), parts along dimension 0, may hold values from -140 to 140, as said below
- mix_gain: bfloat16 [2, 2048], replicated, may hold values from 0.099609375 to 1.8984375
- gate_weight: bfloat16 [2, 2048, 2048], P(None, 'sp', 'tp'), may hold values from -0.125 to 0.125
- mix_weight: bfloat16 [2, 2048, 2048], P(None, 'sp', 'tp'), may hold values from -0.125 to 0.125
- value_weight: bfloat16 [2, 2048, 2048], P(None, 'sp', 'tp'), may hold values from -0.125 to 0.125
- out_weight: bfloat16 [2, 2048, 2048], P(None, 'sp', 'tp'), may hold values from -0.125 to 0.125
- conv_taps: bfloat16 [2, 3, 2048], P(None, None, 'tp'), may hold values from -3.5 to 3.5
Outputs:
- result_stream: bfloat16 [4096, 2048], P(('grp', 'sp'), 'tp'), parts along dimension 0
The draws below stay inside these ranges and needn't reach their ends.
There are 2 independent parts, one for each index of `grp`. The reference program is written for one: setup_inputs(seed, part) draws one part's arguments, and reference() takes and returns one part's arrays. A program takes and returns all parts, laid end to end along the dimension named above; an argument that names none is the same for every part. Nothing has to cross between parts.
Inputs may be any that keep to these rules, and one draw needn't show every extreme that they name: `tokens`: activations with feature scales of several sizes.
All inputs are finite; a program needn't handle non-finite values.
Results may differ from the reference program's by a relative error of at most 0.015.
Values may be sent and summed in bfloat16 or wider, within the bound.
A program may use at most 64 MiB of HBM per device.

```python
import jax
import jax.numpy as jnp
from jax import lax

D = 2048
TAPS = 3
LAYERS = 2
TOKENS = 2048


def draw_tokens(key, part):
    subkeys = jax.random.split(key, 2)
    normal_part = jnp.clip(jax.random.normal(subkeys[0], (TOKENS, D), jnp.float32), -6.0, 6.0)
    column = 10.0 ** (jax.random.uniform(subkeys[1], (D,), jnp.float32) - 0.5)
    column = column * 3.0 ** (jnp.arange(D, dtype=jnp.float32) / D - 0.5)
    return (normal_part * column).astype(jnp.bfloat16)


def levels(rng, shape, cuts, least, top_value):
    gain, own = 1.0, jax.random.fold_in(rng, 6)
    for position, parts in cuts:
        draws = jnp.exp(jax.random.uniform(jax.random.fold_in(own, position), (parts,), jnp.float32, least / len(cuts), top_value / len(cuts)))
        gain = gain * jnp.repeat(draws, shape[position] // parts).reshape([-1 if axis == position else 1 for axis in range(len(shape))])
    return gain


def scatter_about(own_key, shape, scale, reach, pieces=(), kind=jnp.bfloat16):
    entries = jax.random.normal(own_key, shape, jnp.float32) * scale
    if len(pieces) > 0:
        entries = levels(own_key, shape, pieces, -0.22, 0.18) * entries
    return jnp.clip(entries, min=-reach, max=reach).astype(kind)


def setup_inputs(seed: int = 0, part: int = 0) -> dict:
    arg_keys = jax.random.split(jax.random.key(seed), 8)
    own_keys = jax.random.split(jax.random.fold_in(arg_keys[7], part), 8)
    tokens = draw_tokens(jax.random.fold_in(jax.random.fold_in(arg_keys[7], part), 71), part)
    mix_gain = jnp.clip(1.0 + 0.18 * jax.random.normal(arg_keys[1], (LAYERS, D), jnp.float32), 0.099609375, 1.8984375).astype(jnp.bfloat16)
    gate_weight = scatter_about(arg_keys[2], (LAYERS, D, D), D ** -0.5, 0.125, ((1, 4), (2, 4)))
    mix_weight = scatter_about(arg_keys[3], (LAYERS, D, D), D ** -0.5, 0.125, ((1, 4), (2, 4)))
    value_weight = scatter_about(arg_keys[4], (LAYERS, D, D), D ** -0.5, 0.125, ((1, 4), (2, 4)))
    out_weight = scatter_about(arg_keys[5], (LAYERS, D, D), D ** -0.5, 0.125, ((1, 4), (2, 4)))
    conv_taps = scatter_about(arg_keys[6], (LAYERS, TAPS, D), TAPS ** -0.5, 3.5, ((2, 4),))
    return {"tokens": tokens, "mix_gain": mix_gain, "gate_weight": gate_weight, "mix_weight": mix_weight, "value_weight": value_weight, "out_weight": out_weight, "conv_taps": conv_taps}


EPS = 1e-06

def reference(tokens, mix_gain, gate_weight, mix_weight, value_weight, out_weight, conv_taps):
    stream = tokens
    for layer_index in range(LAYERS):
        wide_rows = stream.astype(jnp.float32)
        factor = lax.rsqrt(lax.optimization_barrier(jnp.mean(wide_rows * wide_rows, axis=1, keepdims=True)) + EPS)
        normed = (wide_rows * factor * mix_gain[layer_index].astype(jnp.float32)).astype(jnp.bfloat16)
        gate = jnp.dot(normed, gate_weight[layer_index], preferred_element_type=jnp.float32).astype(jnp.bfloat16)
        inner = jnp.dot(normed, mix_weight[layer_index], preferred_element_type=jnp.float32).astype(jnp.bfloat16)
        values = jnp.dot(normed, value_weight[layer_index], preferred_element_type=jnp.float32).astype(jnp.bfloat16)
        carried = inner.astype(jnp.float32) * values.astype(jnp.float32)
        padded = jnp.pad(carried, ((TAPS - 1, 0), (0, 0)))
        row_count = carried.shape[0]
        tap_rows = conv_taps[layer_index].astype(jnp.float32)
        conv = jnp.zeros_like(carried)
        for tap_index in range(TAPS):
            conv = conv + tap_rows[tap_index] * padded[tap_index:tap_index + row_count]
        mixed = (gate.astype(jnp.float32) * conv).astype(jnp.bfloat16)
        product = jnp.dot(mixed, out_weight[layer_index], preferred_element_type=jnp.float32)
        stream = (wide_rows + product).astype(jnp.bfloat16)
    return stream
```

```python
import functools

import jax
import jax.numpy as jnp
from jax import lax
from jax.experimental import pallas as pl
from jax.experimental.pallas import tpu as pltpu
from jax.sharding import PartitionSpec as P

EPS = 1e-06
KINDS = 4
HALO = 16
PAD = 16
MESH = pl.DeviceIdType.MESH


def when(condition):
    if condition is True:
        return lambda body: body()
    if condition is False:
        return lambda body: None
    return pl.when(condition)


def kernel(sizes, tokens, gain, gate_w, mix_w, value_w, out_w, taps, result,
           wide, acts, tokens_all, normed, carried, gates, mixed, resid, edge_out, edge_in, last, swap_in,
           local_sem, w_send, w_recv, a_send, a_recv, e_send, e_recv, r_send, r_recv, t_send, t_recv, m_send, m_recv):
    groups, n, tps, lows = sizes
    highs = tps // lows
    rows, block_width = tokens.shape
    layers = gate_w.shape[0]
    depth = gate_w.shape[1]
    width = block_width // groups
    reach = edge_in.shape[2]
    total = layers * KINDS
    chunk = min(rows, 256)
    parts = range(groups)
    me, my_grp, my_tp = lax.axis_index("sp"), lax.axis_index("grp"), lax.axis_index("tp")
    my_high, my_low = my_tp // lows, lax.rem(my_tp, lows)

    def tp_at(high, low):
        return lax.rem(high + highs, highs) * lows + low

    x_next, x_prev = {"tp": tp_at(my_high + 1, my_low)}, {"tp": tp_at(my_high - 1 + highs, my_low)}
    across = {"grp": lax.rem(my_grp + 1, groups)}
    sibling = {"tp": my_high * lows + (1 - my_low)}
    right, left = {"sp": me + 1}, {"sp": me - 1}

    lower = 2 * me < n
    step = jnp.where(lower, 1, -1)
    inner, outer = {"sp": me + step}, {"sp": me - step}
    is_end = (me == 0) | (me == n - 1)
    helper = True if n == 4 else (me == 1) | (me == n - 2)
    outer_max = 1 if n == 4 else jnp.where(lower, me, n - 1 - me)
    inner_max = n - 1 - outer_max

    barrier = pltpu.get_barrier_semaphore()
    fixed = []
    if highs > 1:
        fixed.append(x_next)
    if highs > 2:
        fixed.append(x_prev)
    if groups > 1:
        fixed.append(across)
    if lows > 1:
        fixed.append(sibling)
    for device in fixed:
        pl.semaphore_signal(barrier, inc=1, device_id=device, device_id_type=MESH)

    @pl.when(me > 0)
    def _():
        pl.semaphore_signal(barrier, inc=1, device_id=left, device_id_type=MESH)

    @pl.when(me < n - 1)
    def _():
        pl.semaphore_signal(barrier, inc=1, device_id=right, device_id_type=MESH)

    weights = (gate_w, mix_w, value_w, out_w)
    own_columns = pl.ds(pl.multiple_of(my_grp * width, width), width)

    def w_rows(origin):
        return pl.ds(pl.multiple_of(origin * depth, depth), depth)

    def token_place(g, t, offset, size):
        return (pl.ds(pl.multiple_of(g * rows + offset, 8), size),
                pl.ds(pl.multiple_of(t * block_width, block_width), block_width))

    def columns_of(g, t):
        return pl.ds(pl.multiple_of(t * block_width + g * width, width), width)

    own = columns_of(my_grp, my_tp)
    own_slot = jnp.where(me == 1, 1, 0)
    guest_slot = 1 - own_slot
    my_slot = jnp.where(is_end, jnp.where(me == 0, 0, 1), own_slot)

    locals_ = [pltpu.make_async_copy(
        tokens, tokens_all.at[(my_slot,) + token_place(my_grp, my_tp, 0, rows)], local_sem.at[0])]
    for m in range(total):
        locals_.append(pltpu.make_async_copy(
            weights[m % KINDS].at[m // KINDS, :, own_columns], wide.at[m, w_rows(me), :], local_sem.at[m + 1]))
    for copy in locals_:
        copy.start()
    for copy in locals_[:4]:
        copy.wait()

    pl.semaphore_wait(barrier, len(fixed) + jnp.minimum(me, 1) + jnp.minimum(n - 1 - me, 1))

    def w_copy(m, origin, way):
        ref = wide.at[m, w_rows(origin), :]
        return pltpu.make_async_remote_copy(
            src_ref=ref, dst_ref=ref, send_sem=w_send.at[m, way, origin], recv_sem=w_recv.at[m, origin],
            device_id=inner if way == 0 else outer, device_id_type=MESH)

    def gather(sems, place, size, sends):
        top = size // 2
        top -= top % 16
        spans = ((0, top), (top, size - top))
        lane = {"next": 0}

        def copy(origin_grp, origin_tp, span, device, slot):
            ref = place(origin_grp, origin_tp, span[0], span[1])
            return pltpu.make_async_remote_copy(
                src_ref=ref, dst_ref=ref, send_sem=a_send.at[sems, slot], recv_sem=a_recv.at[sems, slot],
                device_id=device, device_id_type=MESH)

        def send(g, s, span, device, slot):
            def described():
                return copy(lax.rem(my_grp + g, groups), tp_at(my_high - s + highs, my_low), span, device, slot)

            described().start()
            sends.append(described)

        def arrived(g, s, span, slot, low=None):
            low = my_low if low is None else low
            copy(lax.rem(my_grp + g, groups), tp_at(my_high - s + highs, low), span, x_next, slot).wait_recv()

        whole = (0, size)
        expected = []

        def to_sibling(g, s, span):
            if lows > 1:
                slot = lane["next"]
                lane["next"] += 1
                send(g, s, span, sibling, slot)
                expected.append((g, s, span, slot))

        x_slot = 5 * highs
        y_slot = x_slot + highs
        top_slot, low_slot = y_slot + 1, y_slot + 1 + highs

        def start():
            if highs > 1:
                send(0, 0, whole, x_next, x_slot)
            if groups > 1:
                send(0, 0, whole, across, y_slot)
            to_sibling(0, 0, whole)

        def turn():
            for s in range(1, highs):
                arrived(0, s, whole, x_slot + s - 1)
                if groups > 1:
                    send(0, s, spans[0], across, top_slot + s - 1)
                if s < highs - 1:
                    send(0, s, whole, x_next, x_slot + s)
                to_sibling(0, s, whole)
            if groups > 1:
                arrived(1, 0, whole, y_slot)
                if highs > 1:
                    send(1, 0, spans[1], x_next, low_slot)
                to_sibling(1, 0, whole)

        def finish():
            if groups > 1:
                for s in range(1, highs):
                    arrived(1, s, spans[1], low_slot + s - 1)
                    if s < highs - 1:
                        send(1, s, spans[1], x_next, low_slot + s)
                    to_sibling(1, s, spans[1])
                    arrived(1, s, spans[0], top_slot + s - 1)
                    to_sibling(1, s, spans[0])
            for g, s, span, slot in expected:
                arrived(g, s, span, slot, 1 - my_low)

        return start, turn, finish

    def token_gather(slot, sems, sends):
        return gather(sems, lambda g, t, offset, size: tokens_all.at[(slot,) + token_place(g, t, offset, size)],
                      rows, sends)

    def part_gather(index, part, halo, sends):
        size = rows + halo

        def place(g, t, offset, size_):
            return acts.at[index, pl.ds(part * size + offset, size_), columns_of(g, t)]

        return gather(2 + index * groups + part, place, size, sends)

    def normalize(x, layer):
        x = x.astype(jnp.float32)
        factor = lax.rsqrt(jnp.mean(x * x, axis=1, keepdims=True) + EPS)
        return (x * factor * gain[layer : layer + 1, :].astype(jnp.float32)).astype(jnp.bfloat16)

    def dot(a, b):
        return jnp.dot(a, b, preferred_element_type=jnp.float32)

    def project(x, first, g, at, size):
        gates[g, pl.ds(at, size), :] = dot(x, wide[first]).astype(jnp.bfloat16)
        inner_ = dot(x, wide[first + 1]).astype(jnp.bfloat16)
        values = dot(x, wide[first + 2]).astype(jnp.bfloat16)
        carried[g, pl.ds(PAD + at, size), :] = inner_.astype(jnp.float32) * values.astype(jnp.float32)

    def convolve(layer, g, at):
        conv = jnp.zeros((rows, width), jnp.float32)
        for tap in range(reach + 1):
            row = taps[layer, tap : tap + 1, own_columns].astype(jnp.float32)
            conv = conv + row * carried[g, PAD + at - reach + tap : PAD + at - reach + tap + rows, :]
        return (gates[g, at : at + rows, :].astype(jnp.float32) * conv).astype(jnp.bfloat16)

    def edge(layer, g):
        return pltpu.make_async_remote_copy(
            src_ref=edge_out.at[layer, g], dst_ref=edge_in.at[layer, g], send_sem=e_send.at[layer, g],
            recv_sem=e_recv.at[layer, g], device_id=right, device_id_type=MESH)

    def zero_edge(g, at):
        carried[g, PAD + at - reach : PAD + at, :] = jnp.zeros((reach, width), jnp.float32)

    def take_edge(layer, g, at):
        edge(layer, g).wait_recv()
        carried[g, PAD + at - reach : PAD + at, :] = edge_in[layer, g]

    def guest_mixed(g, slot):
        return pltpu.make_async_remote_copy(
            src_ref=mixed.at[g, pl.ds(pl.multiple_of(slot * rows, rows), rows), :],
            dst_ref=acts.at[0, pl.ds(g * rows, rows), own], send_sem=m_send.at[g], recv_sem=m_recv.at[g],
            device_id=outer, device_id_type=MESH)

    def later_layers(halo, ends, sends, going, need, hook):
        size = rows + halo
        first_size = chunk + halo
        spans = [(0, first_size)] + [(first_size + i * chunk, chunk) for i in range(rows // chunk - 1)]
        for layer in range(layers):
            index, first = 2 * layer, layer * KINDS
            top = layer == layers - 1
            coming = [None if top else part_gather(index + 1, g, halo, sends) for g in parts]
            for g in parts:
                hook(layer, "turn", g)
                going[g][1]()
            for g in parts:
                hook(layer, "finish", g)
                going[g][2]()
                need(first + 3)
                begin = halo if top else 0
                if not top:
                    for at, count in spans:
                        product = dot(acts[index, g * size + at : g * size + at + count, :], wide[first + 3])
                        stream = (resid[g, at : at + count, :].astype(jnp.float32) + product).astype(jnp.bfloat16)
                        resid[g, at : at + count, :] = stream
                        acts[index + 1, g * size + at : g * size + at + count, own] = stream
                    coming[g][0]()
                else:
                    @pl.loop(0, rows // chunk)
                    def _(c):
                        picked = pl.ds(pl.multiple_of(g * rows + c * chunk, chunk), chunk)
                        product = dot(acts[index, picked, :], wide[first + 3])
                        kept = resid[g, pl.ds(pl.multiple_of(halo + c * chunk, 8), chunk), :].astype(jnp.float32)
                        last[picked, :] = (kept + product).astype(jnp.bfloat16)
            if top:
                break
            for g in parts:
                hook(layer, "stream_turn", g)
                coming[g][1]()
            following = layer + 1
            first = following * KINDS
            going = [part_gather(2 * following, g, 0, sends) for g in parts]
            for g in parts:
                hook(layer, "stream_finish", g)
                coming[g][2]()
                for m in range(first, first + 3):
                    need(m)
                for i, (at, count) in enumerate(reversed(spans)):
                    x = acts[index + 1, g * size + at : g * size + at + count, :]
                    project(normalize(x, following), first, g, at, count)
                    if i == 0:
                        at_edge = PAD + size - reach
                        edge_out[following, g] = carried[g, at_edge : at_edge + reach, :]

                        @pl.when((me > 0) & (me < n - 1))
                        def _():
                            edge(following, g).start()
                if ends:
                    @pl.when(me == 0)
                    def _():
                        zero_edge(g, halo)

                @pl.when(me > 1)
                def _():
                    take_edge(following, g, halo)

                acts[2 * following, g * rows : (g + 1) * rows, own] = convolve(following, g, halo)
                going[g][0]()

        mine = pl.ds(pl.multiple_of(my_grp * rows, rows), rows)
        if groups > 1:
            other = lax.rem(my_grp + 1, groups)
            final = pltpu.make_async_remote_copy(
                src_ref=last.at[pl.ds(pl.multiple_of(other * rows, rows), rows), :], dst_ref=swap_in,
                send_sem=r_send, recv_sem=r_recv, device_id=across, device_id_type=MESH)
            final.start()
            result[:, own_columns] = last[mine, :]
            final.wait()
            result[:, pl.ds(pl.multiple_of(other * width, width), width)] = swap_in[...]
        else:
            result[...] = last[...]
        hook(layers, "last", 0)
        for c in sends:
            c().wait_send()

        @pl.when((me > 0) & (me < n - 1))
        def _():
            for layer in range(1, layers):
                for g in parts:
                    edge(layer, g).wait_send()

    assisted = range(3)
    rest = range(3, total)

    @pl.when(is_end)
    def _():
        sends = []
        away = pltpu.make_async_remote_copy(
            src_ref=tokens_all.at[(my_slot,) + token_place(my_grp, my_tp, 0, rows)],
            dst_ref=tokens_all.at[(my_slot,) + token_place(my_grp, my_tp, 0, rows)],
            send_sem=t_send.at[0], recv_sem=t_recv.at[0], device_id=inner, device_id_type=MESH)
        away.start()
        other = lax.rem(my_grp + 1, groups)

        def beside(g, columns_grp):
            ref = tokens_all.at[my_slot, pl.ds(pl.multiple_of(g * rows, rows), rows), columns_of(columns_grp, my_tp)]
            return pltpu.make_async_remote_copy(
                src_ref=ref, dst_ref=ref, send_sem=t_send.at[1], recv_sem=t_recv.at[1], device_id=across,
                device_id_type=MESH)

        if groups > 1:
            beside(my_grp, other).start()
        for m in range(total):
            if m >= 3:
                locals_[m + 1].wait()
            w_copy(m, me, 0).start()
        if groups > 1:
            beside(other, my_grp).wait_recv()
        for g in parts:
            resid[g, 0:rows, :] = tokens_all[my_slot, g * rows : (g + 1) * rows, own]
        going = [part_gather(0, g, 0, sends) for g in parts]
        for g in parts:
            guest_mixed(g, 0).wait_recv()
            going[g][0]()
        needed = set()

        def need(m):
            if m in needed:
                return
            needed.add(m)

            @pl.loop(1, n)
            def _(k):
                w_copy(m, me + step * k, 0).wait_recv()

        later_layers(0, True, sends, going, need, lambda *_: None)
        away.wait_send()
        if groups > 1:
            beside(my_grp, other).wait_send()
        for m in range(total):
            w_copy(m, me, 0).wait_send()

    @pl.when(jnp.logical_not(is_end))
    def _():
        sends = []

        def plain_or_rest(m):
            if m not in assisted:
                return True
            return False if helper is True else jnp.logical_not(helper)

        def own_in(m):
            w_copy(m, me, 0).start()

        def own_out(m):
            @when(plain_or_rest(m))
            def _():
                w_copy(m, me, 1).start()

        def every(limit, low, body):
            if isinstance(limit, int):
                for k in range(low, limit + 1):
                    body(k)
            else:
                for k in range(low, n - 1):
                    pl.when(k <= limit)(functools.partial(body, k))

        def event_out(m):
            def body(k):
                c = w_copy(m, me - step * k, 0)
                c.wait_recv()
                c.start()

            every(outer_max, 1, body)

        def event_in(m, low=1, high=None):
            def body(k):
                c = w_copy(m, me + step * k, 1)
                c.wait_recv()

                @when(plain_or_rest(m))
                def _():
                    c.start()

            every(inner_max if high is None else high, low, body)

        visitors = []
        guest_in = pltpu.make_async_remote_copy(
            src_ref=tokens_all.at[(guest_slot,) + token_place(my_grp, my_tp, 0, rows)],
            dst_ref=tokens_all.at[(guest_slot,) + token_place(my_grp, my_tp, 0, rows)],
            send_sem=t_send.at[0], recv_sem=t_recv.at[0], device_id=outer, device_id_type=MESH)
        start, turn, finish = token_gather(own_slot, 0, sends)
        g_start, g_turn, g_finish = token_gather(guest_slot, 1, visitors)

        def prepare(slot):
            @pl.loop(0, groups * rows // chunk)
            def _(c):
                picked = pl.ds(pl.multiple_of(c * chunk, chunk), chunk)
                normed[slot, picked, :] = normalize(tokens_all[slot, picked, :], 0)

        start()
        for m in assisted:
            own_in(m)
            own_out(m)
        for m in rest:
            locals_[m + 1].wait()
            own_out(m)
        turn()

        @when(helper)
        def _():
            guest_in.wait_recv()
            g_start()

        finish()
        event_out(0)
        for g in parts:
            resid[g, HALO : HALO + rows, :] = tokens_all[own_slot, g * rows : (g + 1) * rows, own]
        prepare(own_slot)
        event_out(1)
        when(helper)(g_turn)
        event_out(2)
        own_in(3)

        @when(helper)
        def _():
            g_finish()
            for g in parts:
                resid[g, 0:HALO, :] = tokens_all[guest_slot, (g + 1) * rows - HALO : (g + 1) * rows, own]
            prepare(guest_slot)

        if helper is not True:
            @pl.when(jnp.logical_not(helper))
            def _():
                for g in parts:
                    resid[g, 0:HALO, :] = jnp.zeros((HALO, width), jnp.bfloat16)
                    acts[0, g * (rows + HALO) : g * (rows + HALO) + HALO, own] = jnp.zeros((HALO, width), jnp.bfloat16)

        for m in assisted:
            event_in(m)
        event_out(3)
        own_in(4)

        going = [part_gather(0, g, HALO, sends) for g in parts]
        size = rows + HALO
        chunks = rows // chunk
        for g in parts:
            def run(slot, skip):
                @pl.loop(0, chunks)
                def _(i):
                    c = chunks - 1 - i
                    x = normed[slot, pl.ds(pl.multiple_of(g * rows + c * chunk, chunk), chunk), :]
                    project(x, 0, g, pl.multiple_of(slot * rows + c * chunk, chunk), chunk)

            def run_upper():
                run(1, 0)

            def run_lower():
                run(0, 0)

            def send_edge():
                at_edge = PAD + own_slot * rows + rows - 8
                edge_out[0, g] = carried[g, pl.ds(pl.multiple_of(at_edge, 8), 8), :][8 - reach :, :]

                @pl.when(me < n - 2)
                def _():
                    edge(0, g).start()

            when(helper)(run_upper)

            @pl.when(me == 1)
            def _():
                send_edge()

            run_lower()

            @pl.when(me != 1)
            def _():
                send_edge()

            @pl.when(me == 1)
            def _():
                zero_edge(g, 0)

            @pl.when(me > 1)
            def _():
                take_edge(0, g, 0)

            mixed[g, 0:rows, :] = convolve(0, g, 0)

            @when(helper)
            def _():
                mixed[g, rows : 2 * rows, :] = convolve(0, g, rows)
                acts[0, g * size : g * size + HALO, own] = mixed[
                    g, pl.ds(pl.multiple_of(guest_slot * rows + rows - HALO, HALO), HALO), :]
                guest_mixed(g, guest_slot).start()

            acts[0, g * size + HALO : (g + 1) * size, own] = mixed[
                g, pl.ds(pl.multiple_of(own_slot * rows, rows), rows), :]
            going[g][0]()

        tasks = [("o", 4), ("w", 5), ("i", 3), ("o", 5), ("w", 6), ("i", 4), ("o", 6), ("w", 7), ("i", 5), ("o", 7),
                 ("i", 6), ("i", 7)]
        assert total == 8
        points = {(0, "turn", 0): 2, (0, "turn", 1): 5, (0, "finish", 0): 5, (0, "finish", 1): 6,
                  (0, "stream_turn", 0): 8, (0, "stream_turn", 1): 9}

        def advance(count):
            while tasks and count > 0:
                kind, m = tasks.pop(0)
                {"o": event_out, "i": event_in, "w": own_in}[kind](m)
                count -= 1

        def hook(layer, what, g):
            done = 12 - len(tasks)
            if (layer, what, g) in points:
                advance(points[layer, what, g] - done)

        def need(m):
            while ("i", m) in tasks or ("o", m) in tasks:
                advance(1)

        later_layers(HALO, False, sends, going, need, hook)
        advance(12)

        @pl.when(me < n - 2)
        def _():
            for g in parts:
                edge(0, g).wait_send()

        @when(helper)
        def _():
            for c in visitors:
                c().wait_send()
            for g in parts:
                guest_mixed(g, guest_slot).wait_send()

        for m in range(total):
            w_copy(m, me, 0).wait_send()
            every(outer_max, 1, lambda k, m=m: w_copy(m, me - step * k, 0).wait_send())

            @when(plain_or_rest(m))
            def _(m=m):
                w_copy(m, me, 1).wait_send()
                every(inner_max, 1, lambda k: w_copy(m, me + step * k, 1).wait_send())


def shards(tokens, mix_gain, gate_weight, mix_weight, value_weight, out_weight, conv_taps):
    groups, n, tps = lax.axis_size("grp"), lax.axis_size("sp"), lax.axis_size("tp")
    assert groups <= 2 and n >= 4
    lows = 2 if tps % 2 == 0 else 1
    highs = tps // lows
    rows, block_width = tokens.shape
    layers, depth, _ = gate_weight.shape
    assert layers == 2
    reach = conv_taps.shape[1] - 1
    width = block_width // groups
    features = tps * block_width
    slots = 5 * highs + 3 * highs + 1
    total = layers * KINDS
    acts = 2 * layers - 1
    anywhere = pl.BlockSpec(memory_space=pl.ANY)
    vmem = pl.BlockSpec(memory_space=pltpu.VMEM)
    dma = pltpu.SemaphoreType.DMA
    return pl.pallas_call(
        functools.partial(kernel, (groups, n, tps, lows)),
        out_shape=jax.ShapeDtypeStruct(tokens.shape, tokens.dtype),
        in_specs=[anywhere, vmem, anywhere, anywhere, anywhere, anywhere, vmem],
        out_specs=vmem,
        scratch_shapes=[
            pltpu.VMEM((total, n * depth, width), jnp.bfloat16),
            pltpu.VMEM((acts, groups * (rows + HALO), features), jnp.bfloat16),
            pltpu.VMEM((2, groups * rows, features), jnp.bfloat16),
            pltpu.VMEM((2, groups * rows, features), jnp.bfloat16),
            pltpu.VMEM((groups, PAD + 2 * rows, width), jnp.float32),
            pltpu.VMEM((groups, 2 * rows, width), jnp.bfloat16),
            pltpu.VMEM((groups, 2 * rows, width), jnp.bfloat16),
            pltpu.VMEM((groups, rows + HALO, width), jnp.bfloat16),
            pltpu.VMEM((layers, groups, reach, width), jnp.float32),
            pltpu.VMEM((layers, groups, reach, width), jnp.float32),
            pltpu.VMEM((groups * rows, width), jnp.bfloat16),
            pltpu.VMEM((rows, width), jnp.bfloat16),
            dma((total + 1,)),
            dma((total, 2, n)),
            dma((total, n)),
            dma((2 + acts * groups, slots)),
            dma((2 + acts * groups, slots)),
            dma((layers, groups)),
            dma((layers, groups)),
            dma,
            dma,
            dma((2,)),
            dma((2,)),
            dma((groups,)),
            dma((groups,)),
        ],
        compiler_params=pltpu.CompilerParams(
            collective_id=0, has_side_effects=True, vmem_limit_bytes=60 * 1024 * 1024
        ),
        name="mixers",
    )(tokens, mix_gain, gate_weight, mix_weight, value_weight, out_weight, conv_taps)


def solution(mesh):
    return jax.shard_map(
        shards,
        mesh=mesh,
        in_specs=(
            P(("grp", "sp"), "tp"),
            P(),
            P(None, "sp", "tp"),
            P(None, "sp", "tp"),
            P(None, "sp", "tp"),
            P(None, "sp", "tp"),
            P(None, None, "tp"),
        ),
        out_specs=P(("grp", "sp"), "tp"),
        check_vma=False,
    )
```

```python
import functools

import jax
import jax.numpy as jnp
from jax import lax
from jax.experimental import pallas as pl
from jax.experimental.pallas import tpu as pltpu
from jax.sharding import PartitionSpec as P

EPS = 1e-06
KINDS = 4
HALO = 16
PAD = 8
MESH = pl.DeviceIdType.MESH
scope = jax.named_scope


def when(condition):
    if condition is True:
        return lambda body: body()
    if condition is False:
        return lambda body: None
    return pl.when(condition)


def gather_sems(highs, fine):
    return 8 * (highs - 1) + 5 if fine else 6 * (highs - 1) + 3


def kernel(sizes, tokens, gain, gate_w, mix_w, value_w, out_w, taps, result,
           wide, acts, deep, tokens_all, halo_all, normed, carried, gates, mixed, resid, last, swap_in,
           local_sem, w_send, w_recv, a_send, a_recv, r_send, r_recv, t_send, t_recv, m_send, m_recv):
    groups, n, tps, lows, gathers, cuts, reach = sizes
    highs = tps // lows
    rows, block_width = tokens.shape
    layers = gate_w.shape[0]
    depth = gate_w.shape[1]
    width = block_width // groups
    half = width // cuts
    total = layers * KINDS
    final_first = total - KINDS
    fine = range(3)
    pieces = [(m, low, half if m in fine else width)
              for m in range(total) for low in range(0, width, half if m in fine else width)]
    lines = len(pieces)

    def line_of(m, cut=0):
        return pieces.index((m, cut * half, half if m in fine else width))

    chunk = min(rows, 256)
    parts = range(groups)
    me, my_grp, my_tp = lax.axis_index("sp"), lax.axis_index("grp"), lax.axis_index("tp")
    my_high, my_low = my_tp // lows, lax.rem(my_tp, lows)

    def tp_at(high, low):
        return lax.rem(high + highs, highs) * lows + low

    x_next, x_prev = {"tp": tp_at(my_high + 1, my_low)}, {"tp": tp_at(my_high - 1 + highs, my_low)}
    across = {"grp": lax.rem(my_grp + 1, groups)}
    sibling = {"tp": my_high * lows + (1 - my_low)}
    right, left = {"sp": me + 1}, {"sp": me - 1}

    lower = 2 * me < n
    step = jnp.where(lower, 1, -1)
    inner, outer = {"sp": me + step}, {"sp": me - step}
    is_end = (me == 0) | (me == n - 1)
    helper = True if n == 4 else (me == 1) | (me == n - 2)
    outer_max = 1 if n == 4 else jnp.where(lower, me, n - 1 - me)
    inner_max = n - 1 - outer_max

    barrier = pltpu.get_barrier_semaphore()
    fixed = []
    if highs > 1:
        fixed.append(x_next)
    if highs > 2:
        fixed.append(x_prev)
    if groups > 1:
        fixed.append(across)
    if lows > 1:
        fixed.append(sibling)
    for device in fixed:
        pl.semaphore_signal(barrier, inc=1, device_id=device, device_id_type=MESH)

    @pl.when(me > 0)
    def _():
        pl.semaphore_signal(barrier, inc=1, device_id=left, device_id_type=MESH)

    @pl.when(me < n - 1)
    def _():
        pl.semaphore_signal(barrier, inc=1, device_id=right, device_id_type=MESH)

    weights = (gate_w, mix_w, value_w, out_w)
    own_columns = pl.ds(pl.multiple_of(my_grp * width, width), width)

    def w_rows(origin):
        return pl.ds(pl.multiple_of(origin * depth, depth), depth)

    def token_place(g, t, offset, size):
        return (pl.ds(pl.multiple_of(g * rows + offset, 8), size),
                pl.ds(pl.multiple_of(t * block_width, block_width), block_width))

    def columns_of(g, t):
        return pl.ds(pl.multiple_of(t * block_width + g * width, width), width)

    own = columns_of(my_grp, my_tp)
    own_slot = jnp.where(me == 1, 1, 0)
    guest_slot = 1 - own_slot
    my_slot = jnp.where(is_end, jnp.where(me == 0, 0, 1), own_slot)

    locals_ = [pltpu.make_async_copy(
        tokens, tokens_all.at[(my_slot,) + token_place(my_grp, my_tp, 0, rows)], local_sem.at[0])]
    loads = [[] for _ in range(total)]
    for m in range(total):
        if final_first <= m < final_first + 3:
            continue
        loads[m].append(pltpu.make_async_copy(
            weights[m % KINDS].at[m // KINDS, :, own_columns], wide.at[m, w_rows(me), :], local_sem.at[m + 1]))
    for piece in range(3 * cuts):
        m, at = final_first + piece // cuts, piece % cuts * half
        source = pl.ds(pl.multiple_of(my_grp * width + piece // 3 * half, half), half)
        loads[m].append(pltpu.make_async_copy(
            weights[piece % 3].at[layers - 1, :, source], wide.at[m, w_rows(me), pl.ds(at, half)],
            local_sem.at[total + 1 + piece]))
    locals_[0].start()
    for copies in loads:
        for copy in copies:
            copy.start()

    def loaded(m):
        for copy in loads[m]:
            copy.wait()

    with scope("loads"):
        locals_[0].wait()
        for m in range(3):
            loaded(m)

    with scope("entry"):
        pl.semaphore_wait(barrier, len(fixed) + jnp.minimum(me, 1) + jnp.minimum(n - 1 - me, 1))

    def w_copy(m, origin, way):
        matrix, low, columns = pieces[m]
        ref = wide.at[matrix, w_rows(origin), low : low + columns]
        return pltpu.make_async_remote_copy(
            src_ref=ref, dst_ref=ref, send_sem=w_send.at[m, way, origin], recv_sem=w_recv.at[m, origin],
            device_id=inner if way == 0 else outer, device_id_type=MESH)

    sem_bases = [0]
    for index in range(gathers):
        sem_bases.append(sem_bases[-1] + gather_sems(highs, index != 2 and index < 3 + 2 * groups))

    def gather(sems, place, size, sends, fine=False):
        top = size // 2
        top = size if size < 64 else top - top % 16
        spans = ((0, top), (top, size - top))
        split = top < size
        whole = (0, size)
        slots = {}

        def slot_of(key):
            return sem_bases[sems] + slots.setdefault(key, len(slots))

        def copy(origin_grp, origin_tp, span, device, key):
            ref = place(origin_grp, origin_tp, span[0], span[1])
            return pltpu.make_async_remote_copy(
                src_ref=ref, dst_ref=ref, send_sem=a_send.at[slot_of(key)], recv_sem=a_recv.at[slot_of(key)],
                device_id=device, device_id_type=MESH)

        def send(g, s, span, device, key):
            def described():
                return copy(lax.rem(my_grp + g, groups), tp_at(my_high - s + highs, my_low), span, device, key)

            described().start()
            sends.append(described)

        def arrived(g, s, span, key, low=None):
            low = my_low if low is None else low
            copy(lax.rem(my_grp + g, groups), tp_at(my_high - s + highs, low), span, x_next, key).wait_recv()

        expected = []

        def to_sibling(g, s, span):
            if lows > 1:
                key = ("sibling", len(expected))
                send(g, s, span, sibling, key)
                expected.append((g, s, span, key))

        x_spans = ((0, spans[0]), (1, spans[1])) if fine else ((0, whole),)
        y_spans = ((1, spans[1]), (0, spans[0])) if fine else ((1, whole),)

        def start():
            for i, span in x_spans:
                if highs > 1:
                    send(0, 0, span, x_next, ("x", 0, i))
            for i, span in y_spans:
                if groups > 1:
                    send(0, 0, span, across, ("y", i))
            to_sibling(0, 0, whole)

        def turn_one(which):
            for s in range(1, highs):
                for i, span in x_spans[which]:
                    arrived(0, s, span, ("x", s - 1, i))
                    if groups > 1 and i == 0:
                        send(0, s, spans[0], across, ("top", s - 1))
                    if s < highs - 1:
                        send(0, s, span, x_next, ("x", s, i))
                    to_sibling(0, s, span)
            if groups > 1:
                for i, span in y_spans[which]:
                    arrived(1, 0, span, ("y", i))
                    if highs > 1 and split and i == 1:
                        send(1, 0, spans[1], x_next, ("low", 0))
                    to_sibling(1, 0, span)

        def turn_first():
            turn_one(slice(0, 1))

        def turn_second():
            turn_one(slice(1, 2))

        def turn():
            turn_first()
            turn_second()

        def finish():
            if groups > 1:
                for s in range(1, highs):
                    if split:
                        arrived(1, s, spans[1], ("low", s - 1))
                        if s < highs - 1:
                            send(1, s, spans[1], x_next, ("low", s))
                        to_sibling(1, s, spans[1])
                    arrived(1, s, spans[0], ("top", s - 1))
                    to_sibling(1, s, spans[0])
            for g, s, span, key in expected:
                arrived(g, s, span, key, 1 - my_low)
            assert len(slots) <= sem_bases[sems + 1] - sem_bases[sems]

        return start, turn, finish, turn_first, turn_second

    def token_gather(slot, sems, sends):
        return gather(sems, lambda g, t, offset, size: tokens_all.at[(slot,) + token_place(g, t, offset, size)],
                      rows, sends, True)

    def halo_gather(sends):
        def place(g, t, offset, size):
            return halo_all.at[pl.ds(pl.multiple_of(g * HALO + offset, HALO), size), token_place(g, t, 0, HALO)[1]]

        return gather(2, place, HALO, sends)

    def cut_columns(g, t, cut):
        return pl.ds(pl.multiple_of(t * block_width + g * width + cut * half, half), half)

    block = rows // groups

    def part_gather(index, part, sends):
        size = rows + HALO

        def place(g, t, offset, size_):
            return acts.at[index, pl.ds(part * size + offset, size_), columns_of(g, t)]

        return gather(3 + index * groups + part, place, size, sends, True)

    def deep_gather(cut, part, sends):
        def place(g, t, offset, size):
            if cut < cuts - 1:
                return deep.at[part, pl.ds(offset, size), cut_columns(g, t, cut)]
            return deep.at[:, pl.ds(part * block + offset, size), cut_columns(g, t, cut)]

        return gather(3 + (2 + cut) * groups + part, place, rows if cut < cuts - 1 else block, sends)

    def normalize(x, layer):
        x = x.astype(jnp.float32)
        factor = lax.rsqrt(jnp.mean(x * x, axis=1, keepdims=True) + EPS)
        return (x * factor * gain[layer : layer + 1, :].astype(jnp.float32)).astype(jnp.bfloat16)

    def dot(a, b):
        return jnp.dot(a, b, preferred_element_type=jnp.float32)

    def project(x, first, g, at, size):
        gates[g, pl.ds(at, size), :] = dot(x, wide[first]).astype(jnp.bfloat16)
        inner_ = dot(x, wide[first + 1]).astype(jnp.bfloat16)
        values = dot(x, wide[first + 2]).astype(jnp.bfloat16)
        carried[g, pl.ds(PAD + at, size), :] = inner_.astype(jnp.float32) * values.astype(jnp.float32)

    def project_first(x, g, at, size):
        if cuts == 1:
            project(x, final_first, g, at, size)
            return
        early = dot(x, wide[final_first]).astype(jnp.bfloat16)
        later = dot(x, wide[final_first + 1]).astype(jnp.bfloat16)
        gates[g, at : at + size, 0:half] = early[:, :half]
        gates[g, at : at + size, half:] = later[:, half:]
        carried[g, PAD + at : PAD + at + size, 0:half] = (
            early[:, half:].astype(jnp.float32) * later[:, :half].astype(jnp.float32))

    def project_second(x, g, at, size):
        both = dot(x, wide[final_first + 2]).astype(jnp.bfloat16)
        carried[g, PAD + at : PAD + at + size, half:] = (
            both[:, :half].astype(jnp.float32) * both[:, half:].astype(jnp.float32))

    def convolve(layer, g, at, size, low, count):
        conv = jnp.zeros((size, count), jnp.float32)
        for tap in range(reach + 1):
            picked = pl.ds(pl.multiple_of(my_grp * width + low, 128), count)
            row = taps[tap, layer : layer + 1, picked].astype(jnp.float32)
            begin = PAD + at - reach + tap
            conv = conv + row * carried[g, begin : begin + size, low : low + count]
        return (gates[g, at : at + size, low : low + count].astype(jnp.float32) * conv).astype(jnp.bfloat16)

    guest_spans = [(0, chunk + HALO)] + [(HALO + i * chunk, chunk) for i in range(1, rows // chunk)]

    def guest_mixed(g, slot, i):
        at, length = guest_spans[i]
        return pltpu.make_async_remote_copy(
            src_ref=mixed.at[g, pl.ds(pl.multiple_of(slot * rows + at, HALO), length), :],
            dst_ref=acts.at[0, pl.ds(g * (HALO + rows) + at, length), own], send_sem=m_send.at[g, i],
            recv_sem=m_recv.at[g, i], device_id=outer, device_id_type=MESH)

    halo_kept = pltpu.make_async_remote_copy(
        src_ref=resid.at[:, rows : rows + HALO, :], dst_ref=resid.at[:, 0:HALO, :], send_sem=t_send.at[3],
        recv_sem=t_recv.at[3], device_id=right, device_id_type=MESH)

    def later_layers(sends, going, need, hook, eager):
        size = rows + HALO
        spans = [(0, chunk + HALO)] + [(HALO + i * chunk, chunk) for i in range(1, rows // chunk)]
        coming = [part_gather(1, g, sends) for g in parts]
        def second_hop(g):
            hook("turn", g)
            with scope(f"turn0_{g}"):
                if g > 0:
                    going[g][3]()
                going[g][4]()

        if not eager:
            for g in parts:
                second_hop(g)
        for g in parts:
            hook("finish", g)
            if eager and g == 0:
                second_hop(g)
            with scope(f"finish0_{g}"):
                going[g][2]()
            if eager and g < groups - 1:
                second_hop(g + 1)
            with scope(f"need0_{g}"):
                need(line_of(3))
            for at, count in spans:
                product = dot(acts[0, g * size + at : g * size + at + count, :], wide[3])
                stream = (resid[g, at : at + count, :].astype(jnp.float32) + product).astype(jnp.bfloat16)
                resid[g, at : at + count, :] = stream
                acts[1, g * size + at : g * size + at + count, own] = stream
            coming[g][0]()
        for g in parts:
            hook("stream_turn", g)
            with scope(f"sturn{g}"):
                coming[g][1]()

        going = {(cut, g): deep_gather(cut, g, sends) for cut in range(cuts) for g in parts}

        def fill(cut, g):
            deep[g, :, cut_columns(my_grp, my_tp, cut)] = convolve(layers - 1, g, HALO, rows, cut * half, half)

        for g in parts:
            hook("stream_finish", g)
            with scope(f"sfinish{g}"):
                coming[g][2]()
            for at, count in spans:
                normed[g, at : at + count, :] = normalize(acts[1, g * size + at : g * size + at + count, :], layers - 1)
            with scope(f"sneed{g}"):
                for m in range(final_first, final_first + (2 if cuts == 2 else 3)):
                    need(line_of(m))
            with scope(f"first{g}"):
                for at, count in spans:
                    project_first(normed[g, at : at + count, :], g, at, count)
                fill(0, g)
            if cuts == 2:
                going[0, g][0]()
        if cuts == 2:
            for g in parts:
                hook("first_turn", g)
                with scope(f"turn1_{g}"):
                    going[0, g][1]()
            hook("second", 0)
            with scope("vneed"):
                need(line_of(final_first + 2))
            with scope("second"):
                for g in parts:
                    for at, count in spans:
                        project_second(normed[g, at : at + count, :], g, at, count)
                    fill(1, g)
        for u in parts:
            going[cuts - 1, u][0]()
        for g in parts:
            hook("second_turn", g)
            with scope(f"turn2_{g}"):
                going[cuts - 1, g][1]()
        if cuts == 2:
            for g in parts:
                with scope(f"finish1_{g}"):
                    going[0, g][2]()

        other = lax.rem(my_grp + 1, groups)
        writes, swaps = [], []
        flushed = 0
        for u in parts:
            hook("second_finish", u)
            with scope(f"finish2_{u}"):
                going[cuts - 1, u][2]()
            with scope(f"oneed{u}"):
                need(line_of(total - 1))
            for group, at in (((other, 0),) if groups > 1 else ()) + ((my_grp, groups - 1),):
                product = dot(deep[group, u * block : (u + 1) * block, :], wide[total - 1])
                kept = resid[group, HALO + u * block : HALO + (u + 1) * block, :].astype(jnp.float32)
                last[at, u] = (kept + product).astype(jnp.bfloat16)
                if groups > 1 and at == 0:
                    swap = pltpu.make_async_remote_copy(
                        src_ref=last.at[0, u], dst_ref=swap_in.at[u], send_sem=r_send.at[u],
                        recv_sem=r_recv.at[u], device_id=across, device_id_type=MESH)
                    swap.start()
                    swaps.append(swap)
            lines_of = pl.ds(u * block, block)
            writes.append(pltpu.make_async_copy(
                last.at[groups - 1, u], result.at[lines_of, own_columns], local_sem.at[total + 1 + 3 * cuts + u]))
            writes[-1].start()
            if u == 0:
                with scope("flush"):
                    flushed = len(sends) // 2
                    for c in sends[:flushed]:
                        c().wait_send()
        with scope("flush"):
            for c in sends[flushed:]:
                c().wait_send()
        for u, swap in enumerate(swaps):
            with scope(f"swap{u}"):
                swap.wait_recv()
            columns = pl.ds(pl.multiple_of(other * width, width), width)
            writes.append(pltpu.make_async_copy(
                swap_in.at[u], result.at[pl.ds(u * block, block), columns],
                local_sem.at[total + 1 + 3 * cuts + groups + u]))
            writes[-1].start()
        hook("last", 0)
        with scope("writes"):
            for swap in swaps:
                swap.wait_send()
            for write in writes:
                write.wait()

    assisted = range(3 * cuts)
    rest = range(3 * cuts, lines)

    @pl.when(is_end)
    def _():
        sends = []
        away = pltpu.make_async_remote_copy(
            src_ref=tokens_all.at[(my_slot,) + token_place(my_grp, my_tp, 0, rows)],
            dst_ref=tokens_all.at[(my_slot,) + token_place(my_grp, my_tp, 0, rows)],
            send_sem=t_send.at[0], recv_sem=t_recv.at[0], device_id=inner, device_id_type=MESH)
        away.start()
        other = lax.rem(my_grp + 1, groups)

        def beside(g, columns_grp):
            ref = tokens_all.at[my_slot, pl.ds(pl.multiple_of(g * rows, rows), rows), columns_of(columns_grp, my_tp)]
            return pltpu.make_async_remote_copy(
                src_ref=ref, dst_ref=ref, send_sem=t_send.at[1], recv_sem=t_recv.at[1], device_id=across,
                device_id_type=MESH)

        if groups > 1:
            beside(my_grp, other).start()
        for m in range(lines):
            if pieces[m][0] >= 3 and pieces[m][1] == 0:
                loaded(pieces[m][0])
            w_copy(m, me, 0).start()
        if groups > 1:
            beside(other, my_grp).wait_recv()
        for g in parts:
            resid[g, HALO : HALO + rows, :] = tokens_all[my_slot, g * rows : (g + 1) * rows, own]

        @pl.when(me == 0)
        def _():
            resid[:, 0:HALO, :] = jnp.zeros((groups, HALO, width), jnp.bfloat16)

        @pl.when(me > 0)
        def _():
            halo_kept.wait_recv()

        going = [part_gather(0, g, sends) for g in parts]
        for g in parts:
            with scope(f"back_{g}"):
                for i in range(len(guest_spans)):
                    guest_mixed(g, 0, i).wait_recv()
            going[g][0]()
            if g == 0:
                going[g][3]()
        needed = set()

        def need(m):
            if m in needed:
                return
            needed.add(m)

            @pl.loop(1, n)
            def _(k):
                w_copy(m, me + step * k, 0).wait_recv()

        later_layers(sends, going, need, lambda *_: None, True)
        away.wait_send()
        if groups > 1:
            beside(my_grp, other).wait_send()
        for m in range(lines):
            w_copy(m, me, 0).wait_send()

    @pl.when(jnp.logical_not(is_end))
    def _():
        sends = []

        def plain_or_rest(m):
            if m not in assisted:
                return True
            return False if helper is True else jnp.logical_not(helper)

        def own_in(m):
            w_copy(m, me, 0).start()

        def own_out(m):
            @when(plain_or_rest(m))
            def _():
                w_copy(m, me, 1).start()

        def every(limit, low, body):
            if isinstance(limit, int):
                for k in range(low, limit + 1):
                    body(k)
            else:
                for k in range(low, n - 1):
                    pl.when(k <= limit)(functools.partial(body, k))

        def event_out(m):
            def body(k):
                c = w_copy(m, me - step * k, 0)
                with scope(f"o{m}"):
                    c.wait_recv()
                c.start()

            every(outer_max, 1, body)

        def event_in(m, low=1, high=None):
            def body(k):
                c = w_copy(m, me + step * k, 1)
                with scope(f"i{m}_{k}"):
                    c.wait_recv()

                @when(plain_or_rest(m))
                def _():
                    c.start()

            every(inner_max if high is None else high, low, body)

        visitors = []
        guest_in = pltpu.make_async_remote_copy(
            src_ref=tokens_all.at[(guest_slot,) + token_place(my_grp, my_tp, 0, rows)],
            dst_ref=tokens_all.at[(guest_slot,) + token_place(my_grp, my_tp, 0, rows)],
            send_sem=t_send.at[0], recv_sem=t_recv.at[0], device_id=outer, device_id_type=MESH)
        start, turn, finish, _, _ = token_gather(own_slot, 0, sends)
        g_start, _, g_finish, g_turn_first, g_turn_second = token_gather(guest_slot, 1, visitors)

        def prepare(slot):
            for g in parts:
                @pl.loop(0, rows // chunk)
                def _(c):
                    x = tokens_all[slot, pl.ds(pl.multiple_of(g * rows + c * chunk, chunk), chunk), :]
                    normed[g, pl.ds(pl.multiple_of(HALO + slot * rows + c * chunk, HALO), chunk), :] = normalize(x, 0)

        mates = []
        h_start, h_turn, h_finish, _, _ = halo_gather(mates)
        halo_there = (pl.ds(pl.multiple_of(my_grp * HALO, HALO), HALO), token_place(my_grp, my_tp, 0, rows)[1])
        halo_out = pltpu.make_async_remote_copy(
            src_ref=tokens_all.at[(own_slot,) + token_place(my_grp, my_tp, rows - HALO, HALO)],
            dst_ref=halo_all.at[halo_there], send_sem=t_send.at[2], recv_sem=t_recv.at[2], device_id=right,
            device_id_type=MESH)

        @pl.when(me < n - 2)
        def _():
            halo_out.start()

        start()
        for m in assisted:
            own_in(m)
            own_out(m)
        for m in rest:
            if pieces[m][1] == 0:
                loaded(pieces[m][0])
            own_out(m)

        @pl.when(me > 1)
        def _():
            halo_out.wait_recv()
            h_start()

        for g in parts:
            carried[g, 0:PAD, :] = jnp.zeros((PAD, width), jnp.float32)

        with scope("tturn"):
            turn()

        @pl.when(me > 1)
        def _():
            h_turn()

        @when(helper)
        def _():
            with scope("guest"):
                guest_in.wait_recv()
            g_start()

        event_out(line_of(0, 0))
        if cuts == 2:
            event_out(line_of(0, 1))
        with scope("tfinish"):
            finish()
        for g in parts:
            resid[g, HALO : HALO + rows, :] = tokens_all[own_slot, g * rows : (g + 1) * rows, own]
        event_out(line_of(1, 0))

        @pl.when(me > 1)
        def _():
            h_finish()
            for g in parts:
                resid[g, 0:HALO, :] = halo_all[g * HALO : (g + 1) * HALO, own]
                normed[g, 0:HALO, :] = normalize(halo_all[g * HALO : (g + 1) * HALO, :], 0)

        @pl.when(me == 1)
        def _():
            for g in parts:
                normed[g, 0:HALO, :] = jnp.zeros((HALO, normed.shape[2]), jnp.bfloat16)

        with scope("prepare"):
            prepare(own_slot)
        if cuts == 2:
            event_out(line_of(1, 1))
        with scope("gturn"):
            when(helper)(g_turn_first)
        event_out(line_of(2, 0))
        if cuts == 2:
            event_out(line_of(2, 1))
        own_in(line_of(3))
        with scope("gturn"):
            when(helper)(g_turn_second)
        @pl.when(me == n - 2)
        def _():
            halo_kept.start()

        for m in assisted[: 2 * len(assisted) // 3]:
            event_in(m)

        @when(helper)
        def _():
            with scope("gfinish"):
                g_finish()
            with scope("gprepare"):
                prepare(guest_slot)

        for m in assisted[2 * len(assisted) // 3 :]:
            event_in(m)

        @pl.when(me == 1)
        def _():
            for g in parts:
                resid[g, 0:HALO, :] = tokens_all[0, (g + 1) * rows - HALO : (g + 1) * rows, own]

        going = [part_gather(0, g, sends) for g in parts]
        size = rows + HALO
        firsts = [(0, chunk + HALO)] + [(HALO + i * chunk, chunk) for i in range(1, rows // chunk)]
        seconds = [(size + i * chunk, chunk) for i in range(rows // chunk)]

        def run(g, spans, low, high):
            for at, length in spans:
                project(normed[g, at : at + length, :], 0, g, at, length)
            mixed[g, low:high, :] = convolve(0, g, low, high - low, 0, width)

        for g in parts:
            for i, (at, length) in enumerate(guest_spans):
                with scope(f"guests{g}"):
                    @pl.when(me == 1)
                    def _():
                        run(g, [(at, length)], at, at + length)

                    @pl.when(me == n - 2)
                    def _():
                        before = firsts[-1:] if i == 0 else []
                        run(g, before + seconds[i : i + 1], rows + at, rows + at + length)

                @when(helper)
                def _():
                    guest_mixed(g, guest_slot, i).start()

        event_out(line_of(3))
        own_in(line_of(4))
        for g in parts:
            with scope(f"owns{g}"):
                @pl.when(me == 1)
                def _():
                    run(g, seconds, size, size + rows)

                @pl.when(me == n - 2)
                def _():
                    run(g, firsts[:-1], 0, rows)

                if n > 4:
                    @pl.when(jnp.logical_not(helper))
                    def _():
                        run(g, firsts, 0, size)

            acts[0, g * size : (g + 1) * size, own] = mixed[
                g, pl.ds(pl.multiple_of(own_slot * rows, rows), size), :]
            going[g][0]()
            if g == groups - 1:
                going[0][3]()

        p = [line_of(m) for m in range(total)]
        order = [("turn", 0, [("o", p[4]), ("w", p[5]), ("i", p[3], 1)]),
                 ("turn", 1, [("o", p[5]), ("w", p[6]), ("i", p[3], 2)]),
                 ("finish", 0, [("o", p[6]), ("w", p[7]), ("i", p[4], 1)]),
                 ("finish", 1, [("o", p[7]), ("i", p[4], 2)]),
                 ("stream_turn", 0, [("i", p[5], 1)]),
                 ("stream_turn", 1, [("i", p[5], 2)]),
                 ("stream_finish", 0, [("i", p[6], 1)]),
                 ("stream_finish", 1, [("i", p[6], 2)]),
                 ("second", 0, [("i", p[7], 1)]),
                 ("first_turn", 1, [("i", p[7], 2)])]
        assert total == 8
        points = {}
        tasks = []
        for what, g, some in order:
            tasks += some
            if some:
                points[what, g] = some[-1]

        def pass_on(kind, m, k=None):
            if kind == "i" and k == 1:
                event_in(m, 1, 1)
            elif kind == "i":
                event_in(m, 2)
            else:
                {"o": event_out, "w": own_in}[kind](m)

        def hook(what, g):
            if (what, g) in points:
                while points[what, g] in tasks:
                    pass_on(*tasks.pop(0))

        def need(m):
            while any(task[1] == m for task in tasks):
                pass_on(*tasks.pop(0))

        @pl.when(me == n - 2)
        def _():
            halo_kept.wait_send()

        later_layers(sends, going, need, hook, False)
        while tasks:
            pass_on(*tasks.pop(0))

        @pl.when(me < n - 2)
        def _():
            halo_out.wait_send()


        @pl.when(me > 1)
        def _():
            for c in mates:
                c().wait_send()

        @when(helper)
        def _():
            for c in visitors:
                c().wait_send()
            for g in parts:
                for i in range(len(guest_spans)):
                    guest_mixed(g, guest_slot, i).wait_send()

        for m in range(lines):
            w_copy(m, me, 0).wait_send()
            every(outer_max, 1, lambda k, m=m: w_copy(m, me - step * k, 0).wait_send())

            @when(plain_or_rest(m))
            def _(m=m):
                w_copy(m, me, 1).wait_send()
                every(inner_max, 1, lambda k: w_copy(m, me + step * k, 1).wait_send())


def shards(tokens, mix_gain, gate_weight, mix_weight, value_weight, out_weight, conv_taps):
    groups, n, tps = lax.axis_size("grp"), lax.axis_size("sp"), lax.axis_size("tp")
    assert groups <= 2 and n >= 4
    lows = 2 if tps % 2 == 0 else 1
    highs = tps // lows
    rows, block_width = tokens.shape
    layers, depth, _ = gate_weight.shape
    assert layers == 2
    reach = conv_taps.shape[1] - 1
    width = block_width // groups
    features = tps * block_width
    total = layers * KINDS
    acts = 2 * layers - 2
    cuts = 2 if width % 256 == 0 else 1
    pieces = total + 3 * (cuts - 1)
    gathers = 3 + (acts + cuts) * groups
    slots = sum(gather_sems(highs, index != 2 and index < 3 + 2 * groups) for index in range(gathers))
    anywhere = pl.BlockSpec(memory_space=pl.ANY)
    vmem = pl.BlockSpec(memory_space=pltpu.VMEM)
    dma = pltpu.SemaphoreType.DMA
    return pl.pallas_call(
        functools.partial(kernel, (groups, n, tps, lows, gathers, cuts, reach)),
        out_shape=jax.ShapeDtypeStruct(tokens.shape, tokens.dtype),
        in_specs=[anywhere, vmem, anywhere, anywhere, anywhere, anywhere, vmem],
        out_specs=anywhere,
        scratch_shapes=[
            pltpu.VMEM((total, n * depth, width), jnp.bfloat16),
            pltpu.VMEM((acts, groups * (rows + HALO), features), jnp.bfloat16),
            pltpu.VMEM((groups, rows, features), jnp.bfloat16),
            pltpu.VMEM((2, groups * rows, features), jnp.bfloat16),
            pltpu.VMEM((groups * HALO, features), jnp.bfloat16),
            pltpu.VMEM((groups, HALO + 2 * rows, features), jnp.bfloat16),
            pltpu.VMEM((groups, PAD + HALO + 2 * rows, width), jnp.float32),
            pltpu.VMEM((groups, HALO + 2 * rows, width), jnp.bfloat16),
            pltpu.VMEM((groups, HALO + 2 * rows, width), jnp.bfloat16),
            pltpu.VMEM((groups, rows + HALO, width), jnp.bfloat16),
            pltpu.VMEM((groups, groups, rows // groups, width), jnp.bfloat16),
            pltpu.VMEM((groups, rows // groups, width), jnp.bfloat16),
            dma((total + 1 + 3 * cuts + 2 * groups,)),
            dma((pieces, 2, n)),
            dma((pieces, n)),
            dma((slots,)),
            dma((slots,)),
            dma((groups,)),
            dma((groups,)),
            dma((4,)),
            dma((4,)),
            dma((groups, max(rows // 256, 1))),
            dma((groups, max(rows // 256, 1))),
        ],
        compiler_params=pltpu.CompilerParams(
            collective_id=0, has_side_effects=True, vmem_limit_bytes=60 * 1024 * 1024
        ),
        name="mixers",
    )(tokens, mix_gain, gate_weight, mix_weight, value_weight, out_weight, jnp.transpose(conv_taps, (1, 0, 2)))


def solution(mesh):
    return jax.shard_map(
        shards,
        mesh=mesh,
        in_specs=(
            P(("grp", "sp"), "tp"),
            P(),
            P(None, "sp", "tp"),
            P(None, "sp", "tp"),
            P(None, "sp", "tp"),
            P(None, "sp", "tp"),
            P(None, None, "tp"),
        ),
        out_specs=P(("grp", "sp"), "tp"),
        check_vma=False,
    )
```

```python
import functools

import jax
import jax.numpy as jnp
from jax import lax
from jax.experimental import pallas as pl
from jax.experimental.pallas import tpu as pltpu
from jax.sharding import PartitionSpec as P

EPS = 1e-06
KINDS = 4
HALO = 16
PAD = 8
MESH = pl.DeviceIdType.MESH
scope = jax.named_scope


def when(condition):
    if condition is True:
        return lambda body: body()
    if condition is False:
        return lambda body: None
    return pl.when(condition)


def gather_sems(highs, fine):
    return 8 * (highs - 1) + 5 if fine else 6 * (highs - 1) + 3


def kernel(sizes, tokens, gain, gate_w, mix_w, value_w, out_w, taps, result,
           wide, acts, deep, tokens_all, halo_all, normed, carried, gates, mixed, resid, last, swap_in,
           local_sem, w_send, w_recv, a_send, a_recv, r_send, r_recv, t_send, t_recv, m_send, m_recv):
    groups, n, tps, lows, gathers, cuts, reach = sizes
    highs = tps // lows
    rows, block_width = tokens.shape
    layers = gate_w.shape[0]
    depth = gate_w.shape[1]
    width = block_width // groups
    half = width // cuts
    total = layers * KINDS
    final_first = total - KINDS
    fine = range(3)
    pieces = [(m, low, half if m in fine else width)
              for m in range(total) for low in range(0, width, half if m in fine else width)]
    lines = len(pieces)

    def line_of(m, cut=0):
        return pieces.index((m, cut * half, half if m in fine else width))

    chunk = min(rows, 256)
    parts = range(groups)
    me, my_grp, my_tp = lax.axis_index("sp"), lax.axis_index("grp"), lax.axis_index("tp")
    my_high, my_low = my_tp // lows, lax.rem(my_tp, lows)

    def tp_at(high, low):
        return lax.rem(high + highs, highs) * lows + low

    x_next, x_prev = {"tp": tp_at(my_high + 1, my_low)}, {"tp": tp_at(my_high - 1 + highs, my_low)}
    across = {"grp": lax.rem(my_grp + 1, groups)}
    sibling = {"tp": my_high * lows + (1 - my_low)}
    right, left = {"sp": me + 1}, {"sp": me - 1}

    lower = 2 * me < n
    step = jnp.where(lower, 1, -1)
    inner, outer = {"sp": me + step}, {"sp": me - step}
    is_end = (me == 0) | (me == n - 1)
    helper = True if n == 4 else (me == 1) | (me == n - 2)
    outer_max = 1 if n == 4 else jnp.where(lower, me, n - 1 - me)
    inner_max = n - 1 - outer_max

    barrier = pltpu.get_barrier_semaphore()
    fixed = []
    if highs > 1:
        fixed.append(x_next)
    if highs > 2:
        fixed.append(x_prev)
    if groups > 1:
        fixed.append(across)
    if lows > 1:
        fixed.append(sibling)
    for device in fixed:
        pl.semaphore_signal(barrier, inc=1, device_id=device, device_id_type=MESH)

    @pl.when(me > 0)
    def _():
        pl.semaphore_signal(barrier, inc=1, device_id=left, device_id_type=MESH)

    @pl.when(me < n - 1)
    def _():
        pl.semaphore_signal(barrier, inc=1, device_id=right, device_id_type=MESH)

    weights = (gate_w, mix_w, value_w, out_w)
    own_columns = pl.ds(pl.multiple_of(my_grp * width, width), width)

    def w_rows(origin):
        return pl.ds(pl.multiple_of(origin * depth, depth), depth)

    def token_place(g, t, offset, size):
        return (pl.ds(pl.multiple_of(g * rows + offset, 8), size),
                pl.ds(pl.multiple_of(t * block_width, block_width), block_width))

    def columns_of(g, t):
        return pl.ds(pl.multiple_of(t * block_width + g * width, width), width)

    own = columns_of(my_grp, my_tp)
    own_slot = jnp.where(me == 1, 1, 0)
    guest_slot = 1 - own_slot
    my_slot = jnp.where(is_end, jnp.where(me == 0, 0, 1), own_slot)

    locals_ = [pltpu.make_async_copy(
        tokens, tokens_all.at[(my_slot,) + token_place(my_grp, my_tp, 0, rows)], local_sem.at[0])]
    loads = [[] for _ in range(total)]
    for m in range(total):
        if final_first <= m < final_first + 3:
            continue
        loads[m].append(pltpu.make_async_copy(
            weights[m % KINDS].at[m // KINDS, :, own_columns], wide.at[m, w_rows(me), :], local_sem.at[m + 1]))
    for piece in range(3 * cuts):
        m, at = final_first + piece // cuts, piece % cuts * half
        source = pl.ds(pl.multiple_of(my_grp * width + piece // 3 * half, half), half)
        loads[m].append(pltpu.make_async_copy(
            weights[piece % 3].at[layers - 1, :, source], wide.at[m, w_rows(me), pl.ds(at, half)],
            local_sem.at[total + 1 + piece]))
    locals_[0].start()
    for copies in loads:
        for copy in copies:
            copy.start()

    def loaded(m):
        for copy in loads[m]:
            copy.wait()

    with scope("loads"):
        locals_[0].wait()
        for m in range(3):
            loaded(m)

    with scope("entry"):
        pl.semaphore_wait(barrier, len(fixed) + jnp.minimum(me, 1) + jnp.minimum(n - 1 - me, 1))

    def w_copy(m, origin, way):
        matrix, low, columns = pieces[m]
        ref = wide.at[matrix, w_rows(origin), low : low + columns]
        return pltpu.make_async_remote_copy(
            src_ref=ref, dst_ref=ref, send_sem=w_send.at[m, way, origin], recv_sem=w_recv.at[m, origin],
            device_id=inner if way == 0 else outer, device_id_type=MESH)

    sem_bases = [0]
    for index in range(gathers):
        sem_bases.append(sem_bases[-1] + gather_sems(highs, index != 2 and index < 3 + 2 * groups))

    def gather(sems, place, size, sends, fine=False):
        top = size // 2
        top = size if size < 64 else top - top % 16
        spans = ((0, top), (top, size - top))
        split = top < size
        whole = (0, size)
        slots = {}

        def slot_of(key):
            return sem_bases[sems] + slots.setdefault(key, len(slots))

        def copy(origin_grp, origin_tp, span, device, key):
            ref = place(origin_grp, origin_tp, span[0], span[1])
            return pltpu.make_async_remote_copy(
                src_ref=ref, dst_ref=ref, send_sem=a_send.at[slot_of(key)], recv_sem=a_recv.at[slot_of(key)],
                device_id=device, device_id_type=MESH)

        def send(g, s, span, device, key):
            def described():
                return copy(lax.rem(my_grp + g, groups), tp_at(my_high - s + highs, my_low), span, device, key)

            described().start()
            sends.append(described)

        def arrived(g, s, span, key, low=None):
            low = my_low if low is None else low
            copy(lax.rem(my_grp + g, groups), tp_at(my_high - s + highs, low), span, x_next, key).wait_recv()

        expected = []

        def to_sibling(g, s, span):
            if lows > 1:
                key = ("sibling", len(expected))
                send(g, s, span, sibling, key)
                expected.append((g, s, span, key))

        x_spans = ((0, spans[0]), (1, spans[1])) if fine else ((0, whole),)
        y_spans = ((1, spans[1]), (0, spans[0])) if fine else ((1, whole),)

        def start():
            for i, span in x_spans:
                if highs > 1:
                    send(0, 0, span, x_next, ("x", 0, i))
            for i, span in y_spans:
                if groups > 1:
                    send(0, 0, span, across, ("y", i))
            to_sibling(0, 0, whole)

        def turn_one(which):
            for s in range(1, highs):
                for i, span in x_spans[which]:
                    arrived(0, s, span, ("x", s - 1, i))
                    if groups > 1 and i == 0:
                        send(0, s, spans[0], across, ("top", s - 1))
                    if s < highs - 1:
                        send(0, s, span, x_next, ("x", s, i))
                    to_sibling(0, s, span)
            if groups > 1:
                for i, span in y_spans[which]:
                    arrived(1, 0, span, ("y", i))
                    if highs > 1 and split and i == 1:
                        send(1, 0, spans[1], x_next, ("low", 0))
                    to_sibling(1, 0, span)

        def turn_first():
            turn_one(slice(0, 1))

        def turn_second():
            turn_one(slice(1, 2))

        def turn():
            turn_first()
            turn_second()

        def finish():
            if groups > 1:
                for s in range(1, highs):
                    if split:
                        arrived(1, s, spans[1], ("low", s - 1))
                        if s < highs - 1:
                            send(1, s, spans[1], x_next, ("low", s))
                        to_sibling(1, s, spans[1])
                    arrived(1, s, spans[0], ("top", s - 1))
                    to_sibling(1, s, spans[0])
            for g, s, span, key in expected:
                arrived(g, s, span, key, 1 - my_low)
            assert len(slots) <= sem_bases[sems + 1] - sem_bases[sems]

        return start, turn, finish, turn_first, turn_second

    def token_gather(slot, sems, sends):
        return gather(sems, lambda g, t, offset, size: tokens_all.at[(slot,) + token_place(g, t, offset, size)],
                      rows, sends, True)

    def halo_gather(sends):
        def place(g, t, offset, size):
            return halo_all.at[pl.ds(pl.multiple_of(g * HALO + offset, HALO), size), token_place(g, t, 0, HALO)[1]]

        return gather(2, place, HALO, sends)

    def cut_columns(g, t, cut):
        return pl.ds(pl.multiple_of(t * block_width + g * width + cut * half, half), half)

    block = rows // groups

    def part_gather(index, part, sends):
        size = rows + HALO

        def place(g, t, offset, size_):
            return acts.at[index, pl.ds(part * size + offset, size_), columns_of(g, t)]

        return gather(3 + index * groups + part, place, size, sends, True)

    def deep_gather(cut, part, sends):
        def place(g, t, offset, size):
            if cut < cuts - 1:
                return deep.at[part, pl.ds(offset, size), cut_columns(g, t, cut)]
            return deep.at[:, pl.ds(part * block + offset, size), cut_columns(g, t, cut)]

        return gather(3 + (2 + cut) * groups + part, place, rows if cut < cuts - 1 else block, sends)

    def normalize(x, layer):
        x = x.astype(jnp.float32)
        factor = lax.rsqrt(jnp.mean(x * x, axis=1, keepdims=True) + EPS)
        return (x * factor * gain[layer : layer + 1, :].astype(jnp.float32)).astype(jnp.bfloat16)

    def dot(a, b):
        return jnp.dot(a, b, preferred_element_type=jnp.float32)

    def project(x, first, g, at, size):
        gates[g, pl.ds(at, size), :] = dot(x, wide[first]).astype(jnp.bfloat16)
        inner_ = dot(x, wide[first + 1]).astype(jnp.bfloat16)
        values = dot(x, wide[first + 2]).astype(jnp.bfloat16)
        carried[g, pl.ds(PAD + at, size), :] = inner_.astype(jnp.float32) * values.astype(jnp.float32)

    def project_first(x, g, at, size):
        if cuts == 1:
            project(x, final_first, g, at, size)
            return
        early = dot(x, wide[final_first]).astype(jnp.bfloat16)
        later = dot(x, wide[final_first + 1]).astype(jnp.bfloat16)
        gates[g, at : at + size, 0:half] = early[:, :half]
        gates[g, at : at + size, half:] = later[:, half:]
        carried[g, PAD + at : PAD + at + size, 0:half] = (
            early[:, half:].astype(jnp.float32) * later[:, :half].astype(jnp.float32))

    def project_second(x, g, at, size):
        both = dot(x, wide[final_first + 2]).astype(jnp.bfloat16)
        carried[g, PAD + at : PAD + at + size, half:] = (
            both[:, :half].astype(jnp.float32) * both[:, half:].astype(jnp.float32))

    def convolve(layer, g, at, size, low, count):
        conv = jnp.zeros((size, count), jnp.float32)
        for tap in range(reach + 1):
            picked = pl.ds(pl.multiple_of(my_grp * width + low, 128), count)
            row = taps[tap, layer : layer + 1, picked].astype(jnp.float32)
            begin = PAD + at - reach + tap
            conv = conv + row * carried[g, begin : begin + size, low : low + count]
        return (gates[g, at : at + size, low : low + count].astype(jnp.float32) * conv).astype(jnp.bfloat16)

    guest_spans = [(0, chunk + HALO)] + [(HALO + i * chunk, chunk) for i in range(1, rows // chunk)]

    def guest_mixed(g, slot, i):
        at, length = guest_spans[i]
        return pltpu.make_async_remote_copy(
            src_ref=mixed.at[g, pl.ds(pl.multiple_of(slot * rows + at, HALO), length), :],
            dst_ref=acts.at[0, pl.ds(g * (HALO + rows) + at, length), own], send_sem=m_send.at[g, i],
            recv_sem=m_recv.at[g, i], device_id=outer, device_id_type=MESH)

    halo_kept = pltpu.make_async_remote_copy(
        src_ref=resid.at[:, rows : rows + HALO, :], dst_ref=resid.at[:, 0:HALO, :], send_sem=t_send.at[3],
        recv_sem=t_recv.at[3], device_id=right, device_id_type=MESH)

    def later_layers(sends, going, need, hook, eager):
        size = rows + HALO
        spans = [(0, chunk + HALO)] + [(HALO + i * chunk, chunk) for i in range(1, rows // chunk)]
        coming = [part_gather(1, g, sends) for g in parts]
        def second_hop(g):
            hook("turn", g)
            with scope(f"turn0_{g}"):
                if g > 0:
                    going[g][3]()
                going[g][4]()

        if not eager:
            for g in parts:
                second_hop(g)
        for g in parts:
            hook("finish", g)
            if eager and g == 0:
                second_hop(g)
            with scope(f"finish0_{g}"):
                going[g][2]()
            if eager and g < groups - 1:
                second_hop(g + 1)
            with scope(f"need0_{g}"):
                need(line_of(3))
            for at, count in spans:
                product = dot(acts[0, g * size + at : g * size + at + count, :], wide[3])
                stream = (resid[g, at : at + count, :].astype(jnp.float32) + product).astype(jnp.bfloat16)
                resid[g, at : at + count, :] = stream
                acts[1, g * size + at : g * size + at + count, own] = stream
            if eager and g > 0:
                with scope(f"sturn{g - 1}"):
                    coming[g - 1][3]()
            coming[g][0]()
        for g in parts:
            hook("stream_turn", g)
            with scope(f"sturn{g}"):
                if not eager or g == groups - 1:
                    coming[g][3]()
                coming[g][4]()

        going = {(cut, g): deep_gather(cut, g, sends) for cut in range(cuts) for g in parts}

        def fill(cut, g, low=0, length=rows):
            deep[g, low : low + length, cut_columns(my_grp, my_tp, cut)] = convolve(
                layers - 1, g, HALO + low, length, cut * half, half)

        for g in parts:
            hook("stream_finish", g)
            with scope(f"sfinish{g}"):
                coming[g][2]()
            for at, count in spans:
                normed[g, at : at + count, :] = normalize(acts[1, g * size + at : g * size + at + count, :], layers - 1)
            with scope(f"sneed{g}"):
                for m in range(final_first, final_first + (2 if cuts == 2 else 3)):
                    need(line_of(m))
            with scope(f"first{g}"):
                for at, count in spans:
                    project_first(normed[g, at : at + count, :], g, at, count)
                fill(0, g)
            if cuts == 2:
                going[0, g][0]()
        if cuts == 2:
            for g in parts:
                hook("first_turn", g)
                with scope(f"turn1_{g}"):
                    going[0, g][1]()
            hook("second", 0)
            with scope("vneed"):
                need(line_of(final_first + 2))
            with scope("second"):
                assert len(spans) == groups
                for u, (at, count) in enumerate(spans):
                    for g in parts:
                        project_second(normed[g, at : at + count, :], g, at, count)
                        fill(1, g, u * block, block)
                    going[1, u][0]()
        else:
            for u in parts:
                going[0, u][0]()
        for g in parts:
            hook("second_turn", g)
            with scope(f"turn2_{g}"):
                going[cuts - 1, g][1]()
        if cuts == 2:
            for g in parts:
                with scope(f"finish1_{g}"):
                    going[0, g][2]()

        other = lax.rem(my_grp + 1, groups)
        writes, swaps = [], []
        flushed = 0
        for u in parts:
            hook("second_finish", u)
            with scope(f"finish2_{u}"):
                going[cuts - 1, u][2]()
            with scope(f"oneed{u}"):
                need(line_of(total - 1))
            for group, at in (((other, 0),) if groups > 1 else ()) + ((my_grp, groups - 1),):
                product = dot(deep[group, u * block : (u + 1) * block, :], wide[total - 1])
                kept = resid[group, HALO + u * block : HALO + (u + 1) * block, :].astype(jnp.float32)
                last[at, u] = (kept + product).astype(jnp.bfloat16)
                if groups > 1 and at == 0:
                    swap = pltpu.make_async_remote_copy(
                        src_ref=last.at[0, u], dst_ref=swap_in.at[u], send_sem=r_send.at[u],
                        recv_sem=r_recv.at[u], device_id=across, device_id_type=MESH)
                    swap.start()
                    swaps.append(swap)
            lines_of = pl.ds(u * block, block)
            writes.append(pltpu.make_async_copy(
                last.at[groups - 1, u], result.at[lines_of, own_columns], local_sem.at[total + 1 + 3 * cuts + u]))
            writes[-1].start()
            if u == 0:
                with scope("flush"):
                    flushed = len(sends) // 2
                    for c in sends[:flushed]:
                        c().wait_send()
        with scope("flush"):
            for c in sends[flushed:]:
                c().wait_send()
        for u, swap in enumerate(swaps):
            with scope(f"swap{u}"):
                swap.wait_recv()
            columns = pl.ds(pl.multiple_of(other * width, width), width)
            writes.append(pltpu.make_async_copy(
                swap_in.at[u], result.at[pl.ds(u * block, block), columns],
                local_sem.at[total + 1 + 3 * cuts + groups + u]))
            writes[-1].start()
        hook("last", 0)
        with scope("writes"):
            for swap in swaps:
                swap.wait_send()
            for write in writes:
                write.wait()

    assisted = range(3 * cuts)
    rest = range(3 * cuts, lines)

    @pl.when(is_end)
    def _():
        sends = []
        away = pltpu.make_async_remote_copy(
            src_ref=tokens_all.at[(my_slot,) + token_place(my_grp, my_tp, 0, rows)],
            dst_ref=tokens_all.at[(my_slot,) + token_place(my_grp, my_tp, 0, rows)],
            send_sem=t_send.at[0], recv_sem=t_recv.at[0], device_id=inner, device_id_type=MESH)
        away.start()
        other = lax.rem(my_grp + 1, groups)

        def beside(g, columns_grp):
            ref = tokens_all.at[my_slot, pl.ds(pl.multiple_of(g * rows, rows), rows), columns_of(columns_grp, my_tp)]
            return pltpu.make_async_remote_copy(
                src_ref=ref, dst_ref=ref, send_sem=t_send.at[1], recv_sem=t_recv.at[1], device_id=across,
                device_id_type=MESH)

        if groups > 1:
            beside(my_grp, other).start()
        for m in range(lines):
            if pieces[m][0] >= 3 and pieces[m][1] == 0:
                loaded(pieces[m][0])
            w_copy(m, me, 0).start()
        if groups > 1:
            beside(other, my_grp).wait_recv()
        for g in parts:
            resid[g, HALO : HALO + rows, :] = tokens_all[my_slot, g * rows : (g + 1) * rows, own]

        @pl.when(me == 0)
        def _():
            resid[:, 0:HALO, :] = jnp.zeros((groups, HALO, width), jnp.bfloat16)

        @pl.when(me > 0)
        def _():
            halo_kept.wait_recv()

        going = [part_gather(0, g, sends) for g in parts]
        for g in parts:
            with scope(f"back_{g}"):
                for i in range(len(guest_spans)):
                    guest_mixed(g, 0, i).wait_recv()
            going[g][0]()
            if g == 0:
                going[g][3]()
        needed = set()

        def need(m):
            if m in needed:
                return
            needed.add(m)

            @pl.loop(1, n)
            def _(k):
                w_copy(m, me + step * k, 0).wait_recv()

        later_layers(sends, going, need, lambda *_: None, True)
        away.wait_send()
        if groups > 1:
            beside(my_grp, other).wait_send()
        for m in range(lines):
            w_copy(m, me, 0).wait_send()

    @pl.when(jnp.logical_not(is_end))
    def _():
        sends = []

        def plain_or_rest(m):
            if m not in assisted:
                return True
            return False if helper is True else jnp.logical_not(helper)

        def own_in(m):
            w_copy(m, me, 0).start()

        def own_out(m):
            @when(plain_or_rest(m))
            def _():
                w_copy(m, me, 1).start()

        def every(limit, low, body):
            if isinstance(limit, int):
                for k in range(low, limit + 1):
                    body(k)
            else:
                for k in range(low, n - 1):
                    pl.when(k <= limit)(functools.partial(body, k))

        def event_out(m):
            def body(k):
                c = w_copy(m, me - step * k, 0)
                with scope(f"o{m}"):
                    c.wait_recv()
                c.start()

            every(outer_max, 1, body)

        def event_in(m, low=1, high=None):
            def body(k):
                c = w_copy(m, me + step * k, 1)
                with scope(f"i{m}_{k}"):
                    c.wait_recv()

                @when(plain_or_rest(m))
                def _():
                    c.start()

            every(inner_max if high is None else high, low, body)

        visitors = []
        guest_in = pltpu.make_async_remote_copy(
            src_ref=tokens_all.at[(guest_slot,) + token_place(my_grp, my_tp, 0, rows)],
            dst_ref=tokens_all.at[(guest_slot,) + token_place(my_grp, my_tp, 0, rows)],
            send_sem=t_send.at[0], recv_sem=t_recv.at[0], device_id=outer, device_id_type=MESH)
        start, turn, finish, _, _ = token_gather(own_slot, 0, sends)
        g_start, _, g_finish, g_turn_first, g_turn_second = token_gather(guest_slot, 1, visitors)

        def prepare(slot):
            for g in parts:
                @pl.loop(0, rows // chunk)
                def _(c):
                    x = tokens_all[slot, pl.ds(pl.multiple_of(g * rows + c * chunk, chunk), chunk), :]
                    normed[g, pl.ds(pl.multiple_of(HALO + slot * rows + c * chunk, HALO), chunk), :] = normalize(x, 0)

        mates = []
        h_start, h_turn, h_finish, _, _ = halo_gather(mates)
        halo_there = (pl.ds(pl.multiple_of(my_grp * HALO, HALO), HALO), token_place(my_grp, my_tp, 0, rows)[1])
        halo_out = pltpu.make_async_remote_copy(
            src_ref=tokens_all.at[(own_slot,) + token_place(my_grp, my_tp, rows - HALO, HALO)],
            dst_ref=halo_all.at[halo_there], send_sem=t_send.at[2], recv_sem=t_recv.at[2], device_id=right,
            device_id_type=MESH)

        @pl.when(me < n - 2)
        def _():
            halo_out.start()

        start()
        for m in assisted:
            own_in(m)
            own_out(m)
        for m in rest:
            if pieces[m][1] == 0:
                loaded(pieces[m][0])
            own_out(m)

        @pl.when(me > 1)
        def _():
            halo_out.wait_recv()
            h_start()

        for g in parts:
            carried[g, 0:PAD, :] = jnp.zeros((PAD, width), jnp.float32)

        with scope("tturn"):
            turn()

        @pl.when(me > 1)
        def _():
            h_turn()

        @when(helper)
        def _():
            with scope("guest"):
                guest_in.wait_recv()
            g_start()

        event_out(line_of(0, 0))
        if cuts == 2:
            event_out(line_of(0, 1))
        with scope("tfinish"):
            finish()
        for g in parts:
            resid[g, HALO : HALO + rows, :] = tokens_all[own_slot, g * rows : (g + 1) * rows, own]
        event_out(line_of(1, 0))

        @pl.when(me > 1)
        def _():
            h_finish()
            for g in parts:
                resid[g, 0:HALO, :] = halo_all[g * HALO : (g + 1) * HALO, own]
                normed[g, 0:HALO, :] = normalize(halo_all[g * HALO : (g + 1) * HALO, :], 0)

        @pl.when(me == 1)
        def _():
            for g in parts:
                normed[g, 0:HALO, :] = jnp.zeros((HALO, normed.shape[2]), jnp.bfloat16)

        with scope("prepare"):
            prepare(own_slot)
        if cuts == 2:
            event_out(line_of(1, 1))
        with scope("gturn"):
            when(helper)(g_turn_first)
        event_out(line_of(2, 0))
        if cuts == 2:
            event_out(line_of(2, 1))
        own_in(line_of(3))
        with scope("gturn"):
            when(helper)(g_turn_second)
        @pl.when(me == n - 2)
        def _():
            halo_kept.start()

        for m in assisted[: 2 * len(assisted) // 3]:
            event_in(m)

        @when(helper)
        def _():
            with scope("gfinish"):
                g_finish()

        for m in assisted[2 * len(assisted) // 3 :]:
            event_in(m)

        @pl.when(me == 1)
        def _():
            for g in parts:
                resid[g, 0:HALO, :] = tokens_all[0, (g + 1) * rows - HALO : (g + 1) * rows, own]

        going = [part_gather(0, g, sends) for g in parts]
        size = rows + HALO
        firsts = [(0, chunk + HALO)] + [(HALO + i * chunk, chunk) for i in range(1, rows // chunk)]
        seconds = [(size + i * chunk, chunk) for i in range(rows // chunk)]

        def run(g, spans, low, high):
            for at, length in spans:
                project(normed[g, at : at + length, :], 0, g, at, length)
            mixed[g, low:high, :] = convolve(0, g, low, high - low, 0, width)

        for g in parts:
            for i, (at, length) in enumerate(guest_spans):
                @when(helper)
                def _():
                    x = tokens_all[guest_slot, g * rows + i * chunk : g * rows + (i + 1) * chunk, :]
                    there = pl.multiple_of(HALO + guest_slot * rows + i * chunk, HALO)
                    normed[g, pl.ds(there, chunk), :] = normalize(x, 0)

                with scope(f"guests{g}"):
                    @pl.when(me == 1)
                    def _():
                        run(g, [(at, length)], at, at + length)

                    @pl.when(me == n - 2)
                    def _():
                        begin, amount = seconds[i]
                        extra = 2 * HALO if i == 0 else 0
                        run(g, [(begin - extra, amount + extra)], rows + at, rows + at + length)

                @when(helper)
                def _():
                    guest_mixed(g, guest_slot, i).start()

        event_out(line_of(3))
        own_in(line_of(4))
        for g in parts:
            with scope(f"owns{g}"):
                @pl.when(me == 1)
                def _():
                    run(g, seconds, size, size + rows)

                @pl.when(me == n - 2)
                def _():
                    run(g, firsts, 0, rows)

                if n > 4:
                    @pl.when(jnp.logical_not(helper))
                    def _():
                        run(g, firsts, 0, size)

            acts[0, g * size : (g + 1) * size, own] = mixed[
                g, pl.ds(pl.multiple_of(own_slot * rows, rows), size), :]
            going[g][0]()
            if g == groups - 1:
                going[0][3]()

        p = [line_of(m) for m in range(total)]
        order = [("turn", 0, [("o", p[4]), ("w", p[5]), ("i", p[3], 1)]),
                 ("turn", 1, [("o", p[5]), ("w", p[6]), ("i", p[3], 2)]),
                 ("finish", 0, [("o", p[6]), ("w", p[7]), ("i", p[4], 1)]),
                 ("finish", 1, [("o", p[7]), ("i", p[4], 2)]),
                 ("stream_turn", 0, [("i", p[5], 1)]),
                 ("stream_turn", 1, [("i", p[5], 2)]),
                 ("stream_finish", 0, [("i", p[6], 1)]),
                 ("stream_finish", 1, [("i", p[6], 2)]),
                 ("second", 0, [("i", p[7], 1)]),
                 ("second_turn", 0, [("i", p[7], 2)])]
        assert total == 8
        points = {}
        tasks = []
        for what, g, some in order:
            tasks += some
            if some:
                points[what, g] = some[-1]

        def pass_on(kind, m, k=None):
            if kind == "i" and k == 1:
                event_in(m, 1, 1)
            elif kind == "i":
                event_in(m, 2)
            else:
                {"o": event_out, "w": own_in}[kind](m)

        def hook(what, g):
            if (what, g) in points:
                while points[what, g] in tasks:
                    pass_on(*tasks.pop(0))

        def need(m):
            while any(task[1] == m for task in tasks):
                pass_on(*tasks.pop(0))

        @pl.when(me == n - 2)
        def _():
            halo_kept.wait_send()

        later_layers(sends, going, need, hook, False)
        while tasks:
            pass_on(*tasks.pop(0))

        @pl.when(me < n - 2)
        def _():
            halo_out.wait_send()


        @pl.when(me > 1)
        def _():
            for c in mates:
                c().wait_send()

        @when(helper)
        def _():
            for c in visitors:
                c().wait_send()
            for g in parts:
                for i in range(len(guest_spans)):
                    guest_mixed(g, guest_slot, i).wait_send()

        for m in range(lines):
            w_copy(m, me, 0).wait_send()
            every(outer_max, 1, lambda k, m=m: w_copy(m, me - step * k, 0).wait_send())

            @when(plain_or_rest(m))
            def _(m=m):
                w_copy(m, me, 1).wait_send()
                every(inner_max, 1, lambda k: w_copy(m, me + step * k, 1).wait_send())


def shards(tokens, mix_gain, gate_weight, mix_weight, value_weight, out_weight, conv_taps):
    groups, n, tps = lax.axis_size("grp"), lax.axis_size("sp"), lax.axis_size("tp")
    assert groups <= 2 and n >= 4
    lows = 2 if tps % 2 == 0 else 1
    highs = tps // lows
    rows, block_width = tokens.shape
    layers, depth, _ = gate_weight.shape
    assert layers == 2
    reach = conv_taps.shape[1] - 1
    width = block_width // groups
    features = tps * block_width
    total = layers * KINDS
    acts = 2 * layers - 2
    cuts = 2 if width % 256 == 0 else 1
    pieces = total + 3 * (cuts - 1)
    gathers = 3 + (acts + cuts) * groups
    slots = sum(gather_sems(highs, index != 2 and index < 3 + 2 * groups) for index in range(gathers))
    anywhere = pl.BlockSpec(memory_space=pl.ANY)
    vmem = pl.BlockSpec(memory_space=pltpu.VMEM)
    dma = pltpu.SemaphoreType.DMA
    return pl.pallas_call(
        functools.partial(kernel, (groups, n, tps, lows, gathers, cuts, reach)),
        out_shape=jax.ShapeDtypeStruct(tokens.shape, tokens.dtype),
        in_specs=[anywhere, vmem, anywhere, anywhere, anywhere, anywhere, vmem],
        out_specs=anywhere,
        scratch_shapes=[
            pltpu.VMEM((total, n * depth, width), jnp.bfloat16),
            pltpu.VMEM((acts, groups * (rows + HALO), features), jnp.bfloat16),
            pltpu.VMEM((groups, rows, features), jnp.bfloat16),
            pltpu.VMEM((2, groups * rows, features), jnp.bfloat16),
            pltpu.VMEM((groups * HALO, features), jnp.bfloat16),
            pltpu.VMEM((groups, HALO + 2 * rows, features), jnp.bfloat16),
            pltpu.VMEM((groups, PAD + HALO + 2 * rows, width), jnp.float32),
            pltpu.VMEM((groups, HALO + 2 * rows, width), jnp.bfloat16),
            pltpu.VMEM((groups, HALO + 2 * rows, width), jnp.bfloat16),
            pltpu.VMEM((groups, rows + HALO, width), jnp.bfloat16),
            pltpu.VMEM((groups, groups, rows // groups, width), jnp.bfloat16),
            pltpu.VMEM((groups, rows // groups, width), jnp.bfloat16),
            dma((total + 1 + 3 * cuts + 2 * groups,)),
            dma((pieces, 2, n)),
            dma((pieces, n)),
            dma((slots,)),
            dma((slots,)),
            dma((groups,)),
            dma((groups,)),
            dma((4,)),
            dma((4,)),
            dma((groups, max(rows // 256, 1))),
            dma((groups, max(rows // 256, 1))),
        ],
        compiler_params=pltpu.CompilerParams(
            collective_id=0, has_side_effects=True, vmem_limit_bytes=60 * 1024 * 1024
        ),
        name="mixers",
    )(tokens, mix_gain, gate_weight, mix_weight, value_weight, out_weight, jnp.transpose(conv_taps, (1, 0, 2)))


def solution(mesh):
    return jax.shard_map(
        shards,
        mesh=mesh,
        in_specs=(
            P(("grp", "sp"), "tp"),
            P(),
            P(None, "sp", "tp"),
            P(None, "sp", "tp"),
            P(None, "sp", "tp"),
            P(None, "sp", "tp"),
            P(None, None, "tp"),
        ),
        out_specs=P(("grp", "sp"), "tp"),
        check_vma=False,
    )
```
